1024 devices in a mesh: grp: 2 (over x), tp: 16 (over z), dp: 32 (over y, core).
Axes of the slice: x: 2, y: 16, z: 16, core: 2. Of those that a mesh axis runs over, the one named last changes fastest.
The devices are a block of a 4x16x16 slice.
Arguments:
- stream: bfloat16 [256, 4096], P('grp', 'dp'), parts along dimension 0, may hold values from -11 to 11
- states: float32 [2, 256, 32, 64, 64], P(None, ('grp', 'dp'), 'tp'), parts along dimension 1, may hold values from -6 to 6
- norm_gain: bfloat16 [2, 4096], P(None, 'dp'), may hold values from 0.099609375 to 1.8984375
- recept_weight: bfloat16 [2, 4096, 2048], P(None, 'dp', 'tp'), may hold values from -0.09375 to 0.09375
- key_weight: bfloat16 [2, 4096, 2048], P(None, 'dp', 'tp'), may hold values from -0.09375 to 0.09375
- value_weight: bfloat16 [2, 4096, 2048], P(None, 'dp', 'tp'), may hold values from -0.09375 to 0.09375
- decay_weight: bfloat16 [2, 4096, 2048], P(None, 'dp', 'tp'), may hold values from -0.09375 to 0.09375
- rate_weight: bfloat16 [2, 4096, 2048], P(None, 'dp', 'tp'), may hold values from -0.09375 to 0.09375
- gate_weight: bfloat16 [2, 4096, 2048], P(None, 'dp', 'tp'), may hold values from -0.09375 to 0.09375
- out_weight: bfloat16 [2, 2048, 4096], P(None, 'tp', 'dp'), may hold values from -0.125 to 0.125
- decay_bias: float32 [2, 2048], P(None, 'tp'), may hold values from -2 to 2
- head_gain: bfloat16 [2, 2048], P(None, 'tp'), may hold values from 0.099609375 to 1.8984375
Outputs:
- new_stream: bfloat16 [256, 4096], P('grp', 'dp'), parts along dimension 0
- new_states: float32 [2, 256, 32, 64, 64], P(None, ('grp', 'dp'), 'tp'), parts along dimension 1
The draws below stay inside these ranges and needn't reach their ends.
There are 2 independent parts, one for each index of `grp`. The reference program is written for one: setup_inputs(seed, part) draws one part's arguments, and reference() takes and returns one part's arrays. A program takes and returns all parts, laid end to end along the dimension named above; an argument that names none is the same for every part. Nothing has to cross between parts.
All inputs are finite; a program needn't handle non-finite values.
Results may differ from the reference program's by a relative error of at most 0.0068.
Values may be sent and summed in bfloat16 or wider, within the bound.
A program may use at most 32 MiB of HBM per device.

```python
import jax
import jax.numpy as jnp
from jax import lax

D = 4096
INNER = 2048
HEAD = 64
HEADS = 32
SEQS = 128


def draw_stream(key, part):
    first, second = jax.random.split(jax.random.fold_in(key, 11), 2)
    columns = jnp.arange(D, dtype=jnp.float32) / D
    rough = jax.random.uniform(second, (D,), jnp.float32, 0.5, 1.5)
    scales = 0.6 * jnp.power(3.0, columns) * rough
    base = jnp.clip(jax.random.normal(first, (SEQS, D), jnp.float32), -4.0, 4.0)
    values = base * scales[None, :]
    return jnp.clip(values, -11.0, 11.0).astype(jnp.bfloat16)


def levels(stream_key, shape, cuts, smallest, high):
    def one(axis_at, blocks):
        draws = jax.random.uniform(jax.random.fold_in(jax.random.fold_in(stream_key, 6), axis_at), (blocks,), jnp.float32, smallest / len(cuts), high / len(cuts))
        return jnp.repeat(jnp.exp(draws), shape[axis_at] // blocks).reshape((-1,) + (1,) * (len(shape) - axis_at - 1))

    level = one(*cuts[0])
    for cut in cuts[1:]:
        level = level * one(*cut)
    return level


def gaussian(rng, dims, deviation, bound, cuts=(), held_as=jnp.bfloat16):
    values = deviation * jax.random.normal(rng, dims, jnp.float32)
    if cuts:
        values = values * levels(rng, dims, cuts, -0.22, 0.18)
    return jnp.clip(values, -bound, bound).astype(held_as)


def setup_inputs(seed: int = 0, part: int = 0) -> dict:
    key_of = jax.random.split(jax.random.key(seed), 13)
    own_keys = jax.random.split(jax.random.fold_in(key_of[12], part), 13)
    stream = draw_stream(jax.random.fold_in(jax.random.fold_in(key_of[12], part), 71), part)
    states = gaussian(own_keys[1], (2, SEQS, HEADS, HEAD, HEAD), 0.5, 6.0, ((1, 32), (2, 16)), jnp.float32)
    norm_gain = jnp.clip(1.0 + 0.18 * jax.random.normal(key_of[2], (2, D), jnp.float32), 0.099609375, 1.8984375).astype(jnp.bfloat16)
    recept_weight = gaussian(key_of[3], (2, D, INNER), D ** -0.5, 0.09375, ((1, 32), (2, 16)))
    key_weight = gaussian(key_of[4], (2, D, INNER), D ** -0.5, 0.09375, ((1, 32), (2, 16)))
    value_weight = gaussian(key_of[5], (2, D, INNER), D ** -0.5, 0.09375, ((1, 32), (2, 16)))
    decay_weight = gaussian(key_of[6], (2, D, INNER), D ** -0.5, 0.09375, ((1, 32), (2, 16)))
    rate_weight = gaussian(key_of[7], (2, D, INNER), D ** -0.5, 0.09375, ((1, 32), (2, 16)))
    gate_weight = gaussian(key_of[8], (2, D, INNER), D ** -0.5, 0.09375, ((1, 32), (2, 16)))
    out_weight = gaussian(key_of[9], (2, INNER, D), INNER ** -0.5, 0.125, ((1, 16), (2, 32)))
    decay_bias = jnp.clip(jax.random.uniform(key_of[10], (2, INNER), jnp.float32, -2.0, 2.0) * levels(key_of[10], (2, INNER), ((1, 16),), -0.4, 0.0), -2.0, 2.0)
    head_gain = jnp.clip(1.0 + 0.18 * jax.random.normal(key_of[11], (2, INNER), jnp.float32), 0.099609375, 1.8984375).astype(jnp.bfloat16)
    return {"stream": stream, "states": states, "norm_gain": norm_gain, "recept_weight": recept_weight, "key_weight": key_weight, "value_weight": value_weight, "decay_weight": decay_weight, "rate_weight": rate_weight, "gate_weight": gate_weight, "out_weight": out_weight, "decay_bias": decay_bias, "head_gain": head_gain}


def run_block(stream, state_blk, gain, weights, out_weight, bias, hgain):
    current = stream.astype(jnp.float32)
    inv_rms = lax.rsqrt(lax.optimization_barrier(jnp.mean(current * current, axis=1, keepdims=True)) + 1e-06)
    normed = (current * gain.astype(jnp.float32)).astype(jnp.bfloat16)
    seqs = stream.shape[0]
    projected = [(jnp.dot(normed, weight, preferred_element_type=jnp.float32) * inv_rms).reshape(seqs, -1, HEAD) for weight in weights]
    recept, key_vec, value_vec, decay_pre, rate_pre, gate_pre = projected
    unit_key = key_vec * lax.rsqrt(lax.optimization_barrier(jnp.sum(key_vec * key_vec, axis=2, keepdims=True)) + 1e-06)
    rate_vec = jax.nn.sigmoid(rate_pre)
    decay = jnp.exp(-0.606531 * jax.nn.sigmoid(bias.reshape(1, -1, HEAD) + decay_pre))
    removed = jnp.einsum('bhij,bhj->bhi', state_blk, unit_key, precision=lax.Precision.HIGHEST)
    new_state = state_blk * decay[:, :, None, :] - removed[..., None] * (unit_key * rate_vec)[:, :, None, :] + value_vec[..., None] * key_vec[:, :, None, :]
    read = jnp.einsum('bhij,bhj->bhi', new_state, recept, precision=lax.Precision.HIGHEST)
    center = read - lax.optimization_barrier(jnp.mean(read, axis=2, keepdims=True))
    normal_read = center * lax.rsqrt(lax.optimization_barrier(jnp.mean(center * center, axis=2, keepdims=True)) + 1e-05)
    gated = normal_read * hgain.astype(jnp.float32).reshape(1, -1, HEAD) * jax.nn.sigmoid(gate_pre)
    mixed = gated.reshape(seqs, -1).astype(jnp.bfloat16)
    branch = jnp.dot(mixed, out_weight, preferred_element_type=jnp.float32)
    return ((current + branch).astype(jnp.bfloat16), new_state)

def reference(stream, states, norm_gain, recept_weight, key_weight, value_weight, decay_weight, rate_weight, gate_weight, out_weight, decay_bias, head_gain):
    current = stream
    fresh_list = []
    for layer in range(2):
        weights = (recept_weight[layer], key_weight[layer], value_weight[layer], decay_weight[layer], rate_weight[layer], gate_weight[layer])
        current, fresh = run_block(current, states[layer], norm_gain[layer], weights, out_weight[layer], decay_bias[layer], head_gain[layer])
        fresh_list.append(fresh)
    return (current, jnp.stack(fresh_list))
```

```python
import functools

import jax
import jax.numpy as jnp
from jax import lax
from jax.experimental import pallas as pl
from jax.experimental.pallas import tpu as pltpu
from jax.sharding import PartitionSpec as P

HEAD = 64
LANES = 128
MESH = pl.DeviceIdType.MESH
F32 = jnp.float32
BF16 = jnp.bfloat16


def rows_of(shape):
    return lax.broadcasted_iota(jnp.int32, shape, 0)


def mix(a, b):
    n = a.shape[0]
    low = (rows_of(a.shape) & 4) == 0
    return (
        jnp.where(low, a, pltpu.roll(b, 4, 0)),
        jnp.where(low, pltpu.roll(a, n - 4, 0), b),
    )


def per_head_sum(t):
    first = lax.broadcasted_iota(jnp.int32, t.shape, 1) < HEAD
    s0 = jnp.sum(jnp.where(first, t, 0.0), axis=1, keepdims=True)
    s1 = jnp.sum(jnp.where(first, 0.0, t), axis=1, keepdims=True)
    return jnp.where(first, s0, s1)


def sigmoid(t):
    return 1.0 / (1.0 + jnp.exp(-t))


def kernel(
    ny,
    nz,
    model,
    stream,
    states,
    gain,
    w0,
    w1,
    w2,
    w3,
    w4,
    w5,
    wout,
    bias,
    hgain,
    out_x,
    out_s,
    xin,
    gbuf,
    wbuf,
    obuf,
    bbuf,
    hbuf,
    sbuf,
    nbuf,
    sy,
    ry,
    my,
    xm,
    sz,
    rz,
    az,
    fx,
    ox,
    load_sem,
    part_send,
    part_recv,
    send_sem,
    recv_sem,
    store_sem,
):
    z = lax.axis_index("tp")
    d = lax.axis_index("dp")
    y = d // 2
    c = lax.rem(d, 2)
    half = 4 * ny

    def y_peer(k):
        return {"dp": lax.rem(y + k, ny) * 2 + c}

    def z_peer(k):
        return {"tp": lax.rem(z + k, nz)}

    partner = {"dp": 2 * y + 1 - c}

    barrier = pltpu.get_barrier_semaphore()

    def greet(n, peer):
        def body(k, carry):
            pl.semaphore_signal(barrier, inc=1, device_id=peer(k), device_id_type=MESH)
            return carry

        lax.fori_loop(1, n, body, 0)

    pl.semaphore_signal(barrier, inc=1, device_id=partner, device_id_type=MESH)
    greet(ny, y_peer)
    greet(nz, z_peer)

    weights = (w0, w1, w2, w3, w4, w5)
    loads = {}

    def load(name, src, dst, k):
        copy = pltpu.make_async_copy(src, dst, load_sem.at[k])
        copy.start()
        loads[name] = copy

    load("x", stream, xin.at[c], 0)
    load("g", gain, gbuf.at[c], 1)
    for r in range(6):
        load(f"w0{r}", weights[r].at[0], wbuf.at[0, c, :, pl.ds(r * LANES, LANES)], 2 + r)
    load("b", bias, bbuf, 8)
    load("h", hgain, hbuf, 9)
    load("s", states, sbuf, 10)
    load("o", wout, obuf.at[c], 11)
    for r in range(6):
        load(f"w1{r}", weights[r].at[1], wbuf.at[1, c, :, pl.ds(r * LANES, LANES)], 12 + r)

    def exchange(src, dst, k):
        return pltpu.make_async_remote_copy(
            src_ref=src,
            dst_ref=dst,
            send_sem=part_send.at[k],
            recv_sem=part_recv.at[k],
            device_id=partner,
            device_id_type=MESH,
        )

    swaps = [
        exchange(xin.at[c], xin.at[c], 0),
        exchange(gbuf.at[c], gbuf.at[c], 1),
        exchange(wbuf.at[0, c], wbuf.at[0, c], 2),
        exchange(obuf.at[c], obuf.at[c], 3),
        exchange(wbuf.at[1, c], wbuf.at[1, c], 4),
        exchange(fx.at[0], fx.at[1], 5),
    ]

    def send_all(n, peer, here, src, dst, k):
        def body(i, carry):
            h = (i + 1) // 2
            off = n // 2 + h * (1 - 2 * lax.rem(i, 2))
            target = lax.rem(here + off, n)
            pltpu.make_async_remote_copy(
                src_ref=src(target),
                dst_ref=dst(n - off),
                send_sem=send_sem.at[k],
                recv_sem=recv_sem.at[k],
                device_id=peer(off),
                device_id_type=MESH,
            ).start()
            return carry

        lax.fori_loop(0, n - 1, body, 0)

    def wait_all(ref, sem):
        pltpu.make_async_copy(ref, ref, sem).wait()

    loads["x"].wait()
    loads["g"].wait()
    for r in range(6):
        loads[f"w0{r}"].wait()
    pl.semaphore_wait(barrier, ny + nz - 1)
    for k in range(3):
        swaps[k].start()
    loads["o"].wait()
    swaps[3].start()
    for r in range(6):
        loads[f"w1{r}"].wait()
    swaps[4].start()
    for k in range(2):
        swaps[k].wait()

    parts = []
    for core in range(2):
        x = xin[core].astype(F32).reshape(ny // 2, 2, 8, LANES)
        p0, p1 = mix(x[:, 0].reshape(half, LANES), x[:, 1].reshape(half, LANES))
        parts.append(jnp.where(c == 0, p0, p1))

    for layer in range(2):
        y_base = 4 * layer
        even, odd = mix(parts[0], parts[1])
        xm[layer, :, 0] = even.reshape(ny // 2, 8, LANES)
        xm[layer, :, 1] = odd.reshape(ny // 2, 8, LANES)

        normed = jnp.concatenate(
            [parts[core] * gbuf[core, layer : layer + 1].astype(F32) for core in range(2)], axis=1
        ).astype(BF16)
        squares = jnp.sum(parts[0] * parts[0] + parts[1] * parts[1], axis=1, keepdims=True)
        squares = jnp.broadcast_to(squares, (half, LANES))
        coarse = squares.astype(BF16).astype(F32)
        fine = squares - coarse
        if layer == 0:
            swaps[2].wait()
        else:
            swaps[4].wait()
        proj = jnp.dot(
            normed, wbuf[layer].reshape(2 * LANES, 6 * LANES), preferred_element_type=F32
        )
        even, odd = mix(
            jnp.concatenate([proj[:, : 3 * LANES], coarse], axis=1),
            jnp.concatenate([proj[:, 3 * LANES :], fine], axis=1),
        )
        sy[layer, :, 0] = even.reshape(ny // 2, 8, 4 * LANES).astype(BF16)
        sy[layer, :, 1] = odd.reshape(ny // 2, 8, 4 * LANES).astype(BF16)
        send_all(
            ny,
            y_peer,
            y,
            lambda t: sy.at[layer, t // 2, lax.rem(t, 2)],
            lambda slot: ry.at[layer, slot],
            y_base,
        )
        if layer == 0:
            loads["b"].wait()
            loads["h"].wait()
            loads["s"].wait()
        total = sy[layer, y // 2, lax.rem(y, 2)].astype(F32)
        wait_all(ry.at[layer, pl.ds(1, ny - 1)], recv_sem.at[y_base])
        for k in range(1, ny):
            total = total + ry[layer, k].astype(F32)

        sq = total[:, 3 * LANES :]
        inv_rms = lax.rsqrt((sq + pltpu.roll(sq, 4, 0)) * (1.0 / model) + 1e-06)
        pr = total[:, : 3 * LANES] * jnp.concatenate([inv_rms] * 3, axis=1)
        lower = pltpu.roll(pr, 4, 0)
        recept, key_vec, value_vec = (pr[:, k * LANES : (k + 1) * LANES] for k in range(3))
        decay_pre, rate_pre, gate_pre = (lower[:, k * LANES : (k + 1) * LANES] for k in range(3))
        unit_key = key_vec * lax.rsqrt(per_head_sum(key_vec * key_vec) + 1e-06)
        key_rate = unit_key * sigmoid(rate_pre)
        decay = jnp.exp(-0.606531 * sigmoid(bbuf[layer : layer + 1] + decay_pre))
        decay_recept = decay * recept
        lhs = jnp.concatenate(
            [
                unit_key[:, :HEAD],
                unit_key[:, HEAD:],
                decay_recept[:, :HEAD],
                decay_recept[:, HEAD:],
            ],
            axis=0,
        )
        found = lax.dot_general(
            lhs,
            sbuf[layer].reshape(8 * HEAD, HEAD),
            (((1,), (1,)), ((), ())),
            precision=lax.Precision.HIGHEST,
            preferred_element_type=F32,
        )
        row = rows_of((8, LANES))
        first = lax.broadcasted_iota(jnp.int32, (8, LANES), 1) < HEAD
        removed = jnp.zeros((8, LANES), F32)
        kept = jnp.zeros((8, LANES), F32)
        for s in range(4):
            blk = found[:, s * LANES : (s + 1) * LANES]
            removed = jnp.where(row == s, jnp.where(first, blk[0:8], blk[8:16]), removed)
            kept = jnp.where(row == s, jnp.where(first, blk[16:24], blk[24:32]), kept)
        read = (
            kept
            - removed * per_head_sum(key_rate * recept)
            + value_vec * per_head_sum(key_vec * recept)
        )
        center = read - per_head_sum(read) * (1.0 / HEAD)
        var = per_head_sum(center * center) * (1.0 / HEAD)
        gated = (
            center
            * lax.rsqrt(var + 1e-05)
            * hbuf[layer : layer + 1].astype(F32)
            * sigmoid(gate_pre)
        )
        gated = jnp.where(row < 4, gated, 0.0)
        gated = jnp.where(lax.rem(y, 2) == 0, gated, pltpu.roll(gated, 4, 0))
        my[layer, y // 2, lax.rem(y, 2)] = gated.astype(BF16)
        mine_y = my.at[layer, y // 2, lax.rem(y, 2)]
        send_all(ny, y_peer, y, lambda t: mine_y, lambda slot: mine_y, y_base + 1)

        removed_t = jnp.transpose(removed)
        value_t = jnp.transpose(value_vec)
        for h in range(2):
            lanes = slice(h * HEAD, (h + 1) * HEAD)
            dec_h, kr_h, key_h = decay[:, lanes], key_rate[:, lanes], key_vec[:, lanes]
            for s in range(4):
                nbuf[layer, s, h] = (
                    sbuf[layer, s, h] * dec_h[s : s + 1]
                    - removed_t[lanes, s : s + 1] * kr_h[s : s + 1]
                    + value_t[lanes, s : s + 1] * key_h[s : s + 1]
                )
        store = pltpu.make_async_copy(nbuf.at[layer], out_s.at[layer], store_sem.at[layer])
        store.start()

        if layer == 0:
            swaps[3].wait()
        wait_all(ry.at[layer, pl.ds(1, ny - 1), :, pl.ds(0, LANES)], recv_sem.at[y_base + 1])
        gathered = (my[layer, :, 0] + my[layer, :, 1]).astype(F32)
        mixed = gathered.reshape(half, LANES).astype(BF16)
        even, odd = mix(
            jnp.dot(mixed, obuf[0, layer], preferred_element_type=F32),
            jnp.dot(mixed, obuf[1, layer], preferred_element_type=F32),
        )
        sz[layer, :, 0] = even.reshape(nz // 2, 8, LANES).astype(BF16)
        sz[layer, :, 1] = odd.reshape(nz // 2, 8, LANES).astype(BF16)
        send_all(
            nz,
            z_peer,
            z,
            lambda t: sz.at[layer, t // 2, lax.rem(t, 2)],
            lambda slot: rz.at[layer, slot],
            y_base + 2,
        )
        total = sz[layer, z // 2, lax.rem(z, 2)].astype(F32)
        wait_all(rz.at[layer, pl.ds(1, nz - 1)], recv_sem.at[y_base + 2])
        for k in range(1, nz):
            total = total + rz[layer, k].astype(F32)
        fresh = xm[layer, z // 2, lax.rem(z, 2)] + total
        az[layer, z // 2, lax.rem(z, 2)] = fresh.astype(BF16)
        mine_z = az.at[layer, z // 2, lax.rem(z, 2)]
        send_all(nz, z_peer, z, lambda t: mine_z, lambda slot: mine_z, y_base + 3)
        wait_all(rz.at[layer, pl.ds(1, nz - 1)], recv_sem.at[y_base + 3])
        parts = list(
            mix(
                az[layer, :, 0].astype(F32).reshape(half, LANES),
                az[layer, :, 1].astype(F32).reshape(half, LANES),
            )
        )

    fx[0] = jnp.where(c == 0, parts[1], parts[0]).astype(BF16)
    swaps[5].start()
    own = jnp.where(c == 0, parts[0], parts[1])
    swaps[5].wait_recv()
    other = fx[1].astype(F32)
    even, odd = mix(jnp.where(c == 0, own, other), jnp.where(c == 0, other, own))
    out = jnp.stack([even.reshape(ny // 2, 8, LANES), odd.reshape(ny // 2, 8, LANES)], axis=1)
    ox[...] = out.reshape(2 * half, LANES).astype(BF16)
    final = pltpu.make_async_copy(ox, out_x, store_sem.at[2])
    final.start()

    swaps[5].wait_send()
    for layer in range(2):
        y_base = 4 * layer
        wait_all(ry.at[layer, pl.ds(1, ny - 1)], send_sem.at[y_base])
        wait_all(ry.at[layer, pl.ds(1, ny - 1), :, pl.ds(0, LANES)], send_sem.at[y_base + 1])
        wait_all(rz.at[layer, pl.ds(1, nz - 1)], send_sem.at[y_base + 2])
        wait_all(rz.at[layer, pl.ds(1, nz - 1)], send_sem.at[y_base + 3])
        pltpu.make_async_copy(nbuf.at[layer], out_s.at[layer], store_sem.at[layer]).wait()
    final.wait()


def per_device(ny, nz, *args):
    stream, states = args[0], args[1]
    anywhere = pl.BlockSpec(memory_space=pl.ANY)
    half = 4 * ny
    model = stream.shape[1] * 2 * ny
    return pl.pallas_call(
        functools.partial(kernel, ny, nz, model),
        out_shape=(
            jax.ShapeDtypeStruct(stream.shape, BF16),
            jax.ShapeDtypeStruct(states.shape, F32),
        ),
        in_specs=[anywhere] * len(args),
        out_specs=(anywhere, anywhere),
        scratch_shapes=[
            pltpu.VMEM((2, *stream.shape), BF16),
            pltpu.VMEM((2, 2, LANES), BF16),
            pltpu.VMEM((2, 2, LANES, 6 * LANES), BF16),
            pltpu.VMEM((2, 2, LANES, LANES), BF16),
            pltpu.VMEM((2, LANES), F32),
            pltpu.VMEM((2, LANES), BF16),
            pltpu.VMEM(states.shape, F32),
            pltpu.VMEM(states.shape, F32),
            pltpu.VMEM((2, ny // 2, 2, 8, 4 * LANES), BF16),
            pltpu.VMEM((2, ny, 8, 4 * LANES), BF16),
            pltpu.VMEM((2, ny // 2, 2, 8, LANES), BF16),
            pltpu.VMEM((2, ny // 2, 2, 8, LANES), F32),
            pltpu.VMEM((2, nz // 2, 2, 8, LANES), BF16),
            pltpu.VMEM((2, nz, 8, LANES), BF16),
            pltpu.VMEM((2, nz // 2, 2, 8, LANES), BF16),
            pltpu.VMEM((2, half, LANES), BF16),
            pltpu.VMEM(stream.shape, BF16),
            pltpu.SemaphoreType.DMA((18,)),
            pltpu.SemaphoreType.DMA((6,)),
            pltpu.SemaphoreType.DMA((6,)),
            pltpu.SemaphoreType.DMA((8,)),
            pltpu.SemaphoreType.DMA((8,)),
            pltpu.SemaphoreType.DMA((3,)),
        ],
        compiler_params=pltpu.CompilerParams(collective_id=0, has_side_effects=True),
    )(*args)


def solution(mesh):
    in_specs = (
        P("grp", "dp"),
        P(None, ("grp", "dp"), "tp", None, None),
        P(None, "dp"),
        P(None, "dp", "tp"),
        P(None, "dp", "tp"),
        P(None, "dp", "tp"),
        P(None, "dp", "tp"),
        P(None, "dp", "tp"),
        P(None, "dp", "tp"),
        P(None, "tp", "dp"),
        P(None, "tp"),
        P(None, "tp"),
    )
    out_specs = (P("grp", "dp"), P(None, ("grp", "dp"), "tp", None, None))
    ny, nz = mesh.shape["dp"] // 2, mesh.shape["tp"]
    return jax.shard_map(
        functools.partial(per_device, ny, nz),
        mesh=mesh,
        in_specs=in_specs,
        out_specs=out_specs,
        check_vma=False,
    )
```

```python
import functools

import jax
import jax.numpy as jnp
from jax import lax
from jax.experimental import pallas as pl
from jax.experimental.pallas import tpu as pltpu
from jax.sharding import PartitionSpec as P

HEAD = 64
LANES = 128
MESH = pl.DeviceIdType.MESH
F32 = jnp.float32
BF16 = jnp.bfloat16


def rows_of(shape):
    return lax.broadcasted_iota(jnp.int32, shape, 0)


def mix(a, b):
    n = a.shape[0]
    low = (rows_of(a.shape) & 4) == 0
    return (
        jnp.where(low, a, pltpu.roll(b, 4, 0)),
        jnp.where(low, pltpu.roll(a, n - 4, 0), b),
    )


def per_head_sum(t):
    first = lax.broadcasted_iota(jnp.int32, t.shape, 1) < HEAD
    s0 = jnp.sum(jnp.where(first, t, 0.0), axis=1, keepdims=True)
    s1 = jnp.sum(jnp.where(first, 0.0, t), axis=1, keepdims=True)
    return jnp.where(first, s0, s1)


def owners_of(nz):
    return min(4, nz // 2)


def sigmoid(t):
    return 1.0 / (1.0 + jnp.exp(-t))


def kernel(
    ny,
    nz,
    model,
    stream,
    states,
    gain,
    w0,
    w1,
    w2,
    w3,
    w4,
    w5,
    wout,
    bias,
    hgain,
    out_x,
    out_s,
    xin,
    gbuf,
    wbuf,
    obuf,
    bbuf,
    hbuf,
    sbuf,
    sy,
    ry,
    my,
    xm,
    sz,
    rz,
    az,
    fx,
    load_sem,
    part_send,
    part_recv,
    send_sem,
    recv_sem,
):
    z = lax.axis_index("tp")
    d = lax.axis_index("dp")
    y = d // 2
    c = lax.rem(d, 2)
    half = 4 * ny
    owners = owners_of(nz)
    step = nz // owners
    mine = lax.rem(z, step)

    def y_peer(k):
        return {"dp": lax.rem(y + k, ny) * 2 + c}

    def z_peer(k):
        return {"tp": lax.rem(z + k, nz)}

    partner = {"dp": 2 * y + 1 - c}

    barrier = pltpu.get_barrier_semaphore()

    def greet(n, peer):
        def body(k, carry):
            pl.semaphore_signal(barrier, inc=1, device_id=peer(k), device_id_type=MESH)
            return carry

        lax.fori_loop(1, n, body, 0)

    pl.semaphore_signal(barrier, inc=1, device_id=partner, device_id_type=MESH)
    greet(ny, y_peer)
    greet(nz, z_peer)

    weights = (w0, w1, w2, w3, w4, w5)
    loads = {}

    def load(name, src, dst, k):
        copy = pltpu.make_async_copy(src, dst, load_sem.at[k])
        copy.start()
        loads[name] = copy

    load("x", stream, xin.at[c], 0)
    load("g", gain, gbuf.at[c], 1)
    for r in range(6):
        load(f"w0{r}", weights[r].at[0], wbuf.at[0, c, :, pl.ds(r * LANES, LANES)], 2 + r)
    load("b", bias, bbuf, 8)
    load("h", hgain, hbuf, 9)
    load("s", states, sbuf, 10)
    load("o", wout, obuf.at[c], 11)
    for r in range(6):
        load(f"w1{r}", weights[r].at[1], wbuf.at[1, c, :, pl.ds(r * LANES, LANES)], 12 + r)

    def exchange(src, dst, k):
        return pltpu.make_async_remote_copy(
            src_ref=src,
            dst_ref=dst,
            send_sem=part_send.at[k],
            recv_sem=part_recv.at[k],
            device_id=partner,
            device_id_type=MESH,
        )

    swaps = [
        exchange(xin.at[c], xin.at[c], 0),
        exchange(gbuf.at[c], gbuf.at[c], 1),
        exchange(wbuf.at[0, c], wbuf.at[0, c], 2),
        exchange(obuf.at[c], obuf.at[c], 3),
        exchange(wbuf.at[1, c], wbuf.at[1, c], 4),
    ]

    def send_all(n, peer, here, src, dst, k):
        def body(i, carry):
            h = (i + 1) // 2
            off = n // 2 + h * (1 - 2 * lax.rem(i, 2))
            target = lax.rem(here + off, n)
            pltpu.make_async_remote_copy(
                src_ref=src(target),
                dst_ref=dst(n - off),
                send_sem=send_sem.at[k],
                recv_sem=recv_sem.at[k],
                device_id=peer(off),
                device_id_type=MESH,
            ).start()
            return carry

        lax.fori_loop(0, n - 1, body, 0)

    def wait_all(ref, sem):
        pltpu.make_async_copy(ref, ref, sem).wait()

    def put_pieces(buf, layer, even, odd):
        for i in range(step // 2):
            for lane, part in enumerate((even, odd)):
                blocks = part.reshape(owners, step // 2, 8, LANES)[:, i]
                buf[layer, 2 * i + lane] = blocks.astype(buf.dtype)

    def take_pieces(pieces):
        pairs = []
        for lane in range(2):
            picked = [pieces[2 * i + lane] for i in range(step // 2)]
            pairs.append(jnp.stack(picked, axis=1).reshape(half, LANES))
        return mix(pairs[0], pairs[1])

    def spread(ref, k, cores):
        for off in sorted(range(1 - step // 2, step // 2 + 1), key=lambda t: -abs(t)):
            for core in cores:
                if off == 0 and core is c:
                    continue
                pltpu.make_async_remote_copy(
                    src_ref=ref,
                    dst_ref=ref,
                    send_sem=send_sem.at[k],
                    recv_sem=recv_sem.at[k],
                    device_id={"tp": lax.rem(z + off + nz, nz), "dp": 2 * y + core},
                    device_id_type=MESH,
                ).start()

    loads["x"].wait()
    loads["g"].wait()
    for r in range(6):
        loads[f"w0{r}"].wait()
    pl.semaphore_wait(barrier, ny + nz - 1)
    for k in range(3):
        swaps[k].start()
    loads["o"].wait()
    swaps[3].start()
    for r in range(6):
        loads[f"w1{r}"].wait()
    swaps[4].start()
    for k in range(2):
        swaps[k].wait()

    parts = []
    for core in range(2):
        x = xin[core].astype(F32).reshape(ny // 2, 2, 8, LANES)
        p0, p1 = mix(x[:, 0].reshape(half, LANES), x[:, 1].reshape(half, LANES))
        parts.append(jnp.where(c == 0, p0, p1))

    for layer in range(2):
        y_base = 4 * layer
        even, odd = mix(parts[0], parts[1])
        put_pieces(xm, layer, even, odd)

        normed = jnp.concatenate(
            [parts[core] * gbuf[core, layer : layer + 1].astype(F32) for core in range(2)], axis=1
        ).astype(BF16)
        squares = jnp.sum(parts[0] * parts[0] + parts[1] * parts[1], axis=1, keepdims=True)
        squares = jnp.broadcast_to(squares, (half, LANES))
        coarse = squares.astype(BF16).astype(F32)
        fine = squares - coarse
        if layer == 0:
            swaps[2].wait()
        else:
            swaps[4].wait()
        proj = jnp.dot(
            normed, wbuf[layer].reshape(2 * LANES, 6 * LANES), preferred_element_type=F32
        )
        even, odd = mix(
            jnp.concatenate([proj[:, : 3 * LANES], coarse], axis=1),
            jnp.concatenate([proj[:, 3 * LANES :], fine], axis=1),
        )
        sy[layer, :, 0] = even.reshape(ny // 2, 8, 4 * LANES).astype(BF16)
        sy[layer, :, 1] = odd.reshape(ny // 2, 8, 4 * LANES).astype(BF16)
        send_all(
            ny,
            y_peer,
            y,
            lambda t: sy.at[layer, t // 2, lax.rem(t, 2)],
            lambda slot: ry.at[layer, slot],
            y_base,
        )
        if layer == 0:
            loads["b"].wait()
            loads["h"].wait()
            loads["s"].wait()
        total = sy[layer, y // 2, lax.rem(y, 2)].astype(F32)
        wait_all(ry.at[layer, pl.ds(1, ny - 1)], recv_sem.at[y_base])
        for k in range(1, ny):
            total = total + ry[layer, k].astype(F32)

        sq = total[:, 3 * LANES :]
        inv_rms = lax.rsqrt((sq + pltpu.roll(sq, 4, 0)) * (1.0 / model) + 1e-06)
        pr = total[:, : 3 * LANES] * jnp.concatenate([inv_rms] * 3, axis=1)
        lower = pltpu.roll(pr, 4, 0)
        recept, key_vec, value_vec = (pr[:, k * LANES : (k + 1) * LANES] for k in range(3))
        decay_pre, rate_pre, gate_pre = (lower[:, k * LANES : (k + 1) * LANES] for k in range(3))
        unit_key = key_vec * lax.rsqrt(per_head_sum(key_vec * key_vec) + 1e-06)
        key_rate = unit_key * sigmoid(rate_pre)
        decay = jnp.exp(-0.606531 * sigmoid(bbuf[layer : layer + 1] + decay_pre))
        decay_recept = decay * recept
        lhs = jnp.concatenate(
            [
                unit_key[:, :HEAD],
                unit_key[:, HEAD:],
                decay_recept[:, :HEAD],
                decay_recept[:, HEAD:],
            ],
            axis=0,
        )
        found = lax.dot_general(
            lhs,
            sbuf[layer].reshape(8 * HEAD, HEAD),
            (((1,), (1,)), ((), ())),
            precision=lax.Precision.HIGHEST,
            preferred_element_type=F32,
        )
        row = rows_of((8, LANES))
        first = lax.broadcasted_iota(jnp.int32, (8, LANES), 1) < HEAD
        removed = jnp.zeros((8, LANES), F32)
        kept = jnp.zeros((8, LANES), F32)
        for s in range(4):
            blk = found[:, s * LANES : (s + 1) * LANES]
            removed = jnp.where(row == s, jnp.where(first, blk[0:8], blk[8:16]), removed)
            kept = jnp.where(row == s, jnp.where(first, blk[16:24], blk[24:32]), kept)
        read = (
            kept
            - removed * per_head_sum(key_rate * recept)
            + value_vec * per_head_sum(key_vec * recept)
        )
        center = read - per_head_sum(read) * (1.0 / HEAD)
        var = per_head_sum(center * center) * (1.0 / HEAD)
        gated = (
            center
            * lax.rsqrt(var + 1e-05)
            * hbuf[layer : layer + 1].astype(F32)
            * sigmoid(gate_pre)
        )
        gated = jnp.where(row < 4, gated, 0.0)
        gated = jnp.where(lax.rem(y, 2) == 0, gated, pltpu.roll(gated, 4, 0))
        my[layer, y // 2, lax.rem(y, 2)] = gated.astype(BF16)
        mine_y = my.at[layer, y // 2, lax.rem(y, 2)]
        send_all(ny, y_peer, y, lambda t: mine_y, lambda slot: mine_y, y_base + 1)

        removed_t = jnp.transpose(removed)
        value_t = jnp.transpose(value_vec)
        for h in range(2):
            lanes = slice(h * HEAD, (h + 1) * HEAD)
            dec_h, kr_h, key_h = decay[:, lanes], key_rate[:, lanes], key_vec[:, lanes]
            for s in range(4):
                out_s[layer, s, h] = (
                    sbuf[layer, s, h] * dec_h[s : s + 1]
                    - removed_t[lanes, s : s + 1] * kr_h[s : s + 1]
                    + value_t[lanes, s : s + 1] * key_h[s : s + 1]
                )

        if layer == 0:
            swaps[3].wait()
        wait_all(ry.at[layer, pl.ds(1, ny - 1), :, pl.ds(0, LANES)], recv_sem.at[y_base + 1])
        gathered = (my[layer, :, 0] + my[layer, :, 1]).astype(F32)
        mixed = gathered.reshape(half, LANES).astype(BF16)
        even, odd = mix(
            jnp.dot(mixed, obuf[0, layer], preferred_element_type=F32),
            jnp.dot(mixed, obuf[1, layer], preferred_element_type=F32),
        )
        put_pieces(sz, layer, even, odd)
        send_all(
            nz,
            z_peer,
            z,
            lambda t: sz.at[layer, lax.rem(t, step)],
            lambda slot: rz.at[layer, slot],
            y_base + 2,
        )
        total = sz[layer, mine].astype(F32)
        wait_all(rz.at[layer, pl.ds(1, nz - 1)], recv_sem.at[y_base + 2])
        for k in range(1, nz):
            total = total + rz[layer, k].astype(F32)
        fresh = (xm[layer, mine] + total).astype(BF16)
        if layer == 0:
            az[mine] = fresh
            spread(az.at[mine], y_base + 3, (c,))
            wait_all(az.at[pl.ds(0, step - 1)], recv_sem.at[y_base + 3])
            parts = list(take_pieces(az[...].astype(F32)))
        else:
            fx[c * step + mine] = fresh
            spread(fx.at[c * step + mine], y_base + 3, (c, 1 - c))
            wait_all(fx.at[pl.ds(0, 2 * step - 1)], recv_sem.at[y_base + 3])

    halves = []
    for core in range(2):
        a, b = take_pieces(fx[core * step : (core + 1) * step].astype(F32))
        halves.append(jnp.where(c == 0, a, b))
    even, odd = mix(halves[0], halves[1])
    out = jnp.stack([even.reshape(ny // 2, 8, LANES), odd.reshape(ny // 2, 8, LANES)], axis=1)
    out_x[...] = out.reshape(2 * half, LANES).astype(BF16)

    for layer in range(2):
        y_base = 4 * layer
        wait_all(ry.at[layer, pl.ds(1, ny - 1)], send_sem.at[y_base])
        wait_all(ry.at[layer, pl.ds(1, ny - 1), :, pl.ds(0, LANES)], send_sem.at[y_base + 1])
        wait_all(rz.at[layer, pl.ds(1, nz - 1)], send_sem.at[y_base + 2])
        spread_wait = az.at[pl.ds(0, step - 1)] if layer == 0 else fx.at[pl.ds(0, 2 * step - 1)]
        wait_all(spread_wait, send_sem.at[y_base + 3])


def write_out(x, s, out_x, out_s, sem):
    copies = [
        pltpu.make_async_copy(x, out_x, sem.at[0]),
        pltpu.make_async_copy(s.at[0], out_s.at[0], sem.at[1]),
        pltpu.make_async_copy(s.at[1], out_s.at[1], sem.at[2]),
    ]
    for copy in copies:
        copy.start()
    for copy in copies:
        copy.wait()


def per_device(ny, nz, *args):
    stream, states = args[0], args[1]
    anywhere = pl.BlockSpec(memory_space=pl.ANY)
    owners = owners_of(nz)
    pieces = (nz // owners, owners, 8, LANES)
    model = stream.shape[1] * 2 * ny
    results = pl.pallas_call(
        functools.partial(kernel, ny, nz, model),
        out_shape=(
            pltpu.VMEM(stream.shape, BF16),
            pltpu.VMEM(states.shape, F32),
        ),
        in_specs=[anywhere] * len(args),
        out_specs=(pl.BlockSpec(memory_space=pltpu.VMEM),) * 2,
        scratch_shapes=[
            pltpu.VMEM((2, *stream.shape), BF16),
            pltpu.VMEM((2, 2, LANES), BF16),
            pltpu.VMEM((2, 2, LANES, 6 * LANES), BF16),
            pltpu.VMEM((2, 2, LANES, LANES), BF16),
            pltpu.VMEM((2, LANES), F32),
            pltpu.VMEM((2, LANES), BF16),
            pltpu.VMEM(states.shape, F32),
            pltpu.VMEM((2, ny // 2, 2, 8, 4 * LANES), BF16),
            pltpu.VMEM((2, ny, 8, 4 * LANES), BF16),
            pltpu.VMEM((2, ny // 2, 2, 8, LANES), BF16),
            pltpu.VMEM((2, *pieces), F32),
            pltpu.VMEM((2, *pieces), BF16),
            pltpu.VMEM((2, nz, *pieces[1:]), BF16),
            pltpu.VMEM(pieces, BF16),
            pltpu.VMEM((2 * pieces[0], *pieces[1:]), BF16),
            pltpu.SemaphoreType.DMA((18,)),
            pltpu.SemaphoreType.DMA((5,)),
            pltpu.SemaphoreType.DMA((5,)),
            pltpu.SemaphoreType.DMA((8,)),
            pltpu.SemaphoreType.DMA((8,)),
        ],
        compiler_params=pltpu.CompilerParams(collective_id=0, has_side_effects=True),
    )(*args)
    inside = pl.BlockSpec(memory_space=pltpu.VMEM)
    return pl.pallas_call(
        write_out,
        out_shape=(
            jax.ShapeDtypeStruct(stream.shape, BF16),
            jax.ShapeDtypeStruct(states.shape, F32),
        ),
        in_specs=[inside, inside],
        out_specs=(anywhere, anywhere),
        scratch_shapes=[pltpu.SemaphoreType.DMA((3,))],
    )(*(pltpu.with_memory_space_constraint(r, pltpu.VMEM) for r in results))


def solution(mesh):
    in_specs = (
        P("grp", "dp"),
        P(None, ("grp", "dp"), "tp", None, None),
        P(None, "dp"),
        P(None, "dp", "tp"),
        P(None, "dp", "tp"),
        P(None, "dp", "tp"),
        P(None, "dp", "tp"),
        P(None, "dp", "tp"),
        P(None, "dp", "tp"),
        P(None, "tp", "dp"),
        P(None, "tp"),
        P(None, "tp"),
    )
    out_specs = (P("grp", "dp"), P(None, ("grp", "dp"), "tp", None, None))
    ny, nz = mesh.shape["dp"] // 2, mesh.shape["tp"]
    return jax.shard_map(
        functools.partial(per_device, ny, nz),
        mesh=mesh,
        in_specs=in_specs,
        out_specs=out_specs,
        check_vma=False,
    )
```
